32 devices in a mesh: ep: 16 (over z, x, core), tp: 2 (over y).
Axes of the slice: x: 2, y: 2, z: 4, core: 2. Of those that a mesh axis runs over, the one named last changes fastest.
Arguments:
- tokens: bfloat16 [256, 2048], P('ep', 'tp'), may hold values from -6 to 6
- state: bfloat16 [256, 32, 4096], P('ep', 'tp'), may hold values from -6 to 6
- mix_gain: float32 [2048], P('tp'), may hold values from 0.1 to 1.9
- w_recept: bfloat16 [2048, 2048], P('tp', 'ep'), may hold values from -0.125 to 0.125
- w_key: bfloat16 [2048, 2048], P('tp', 'ep'), may hold values from -0.125 to 0.125
- w_value: bfloat16 [2048, 2048], P('tp', 'ep'), may hold values from -0.125 to 0.125
- w_decay: bfloat16 [2048, 2048], P('tp', 'ep'), may hold values from -0.125 to 0.125
- w_rate: bfloat16 [2048, 2048], P('tp', 'ep'), may hold values from -0.125 to 0.125
- decay_base: float32 [2048], P('tp'), may hold values from -4 to 2
- rate_base: float32 [2048], P('tp'), may hold values from -2 to 2
- head_gain: float32 [2048], P('tp'), may hold values from 0.1 to 1.9
- w_out: bfloat16 [2048, 2048], P('tp', 'ep'), may hold values from -0.125 to 0.125
- moe_gain: float32 [2048], replicated, may hold values from 0.1 to 1.9
- routes: int32 [256, 6], P('ep'), may hold values from 0 to 15, all different within a row; in each aligned block of 16 rows (0 to 15, 16 to 31, ...) at most 12 rows name the same one
- route_weight: float32 [256, 6], P('ep'), may hold values from 0.1 to 1
- expert_gate: bfloat16 [16, 2048, 512], P('ep', None, 'tp'), may hold values from -0.125 to 0.125
- expert_up: bfloat16 [16, 2048, 512], P('ep', None, 'tp'), may hold values from -0.125 to 0.125
- expert_down: bfloat16 [16, 512, 2048], P('ep', 'tp'), may hold values from -0.25 to 0.25
- shared_gate: bfloat16 [2048, 512], P(None, 'tp'), may hold values from -0.125 to 0.125
- shared_up: bfloat16 [2048, 512], P(None, 'tp'), may hold values from -0.125 to 0.125
- shared_down: bfloat16 [512, 2048], P('tp'), may hold values from -0.25 to 0.25
Outputs:
- layer_out: bfloat16 [256, 2048], P('ep', 'tp')
The draws below stay inside these ranges and needn't reach their ends.
Inputs may be any that keep to these rules, and one draw needn't show every extreme that they name: `routes`: each row names 6 different experts. Within the rows of one device (aligned blocks of 16 rows) no expert is named by more than 12 rows, a bound that some block reaches.
All inputs are finite; a program needn't handle non-finite values.
Results may differ from the reference program's by a relative error of at most 0.024.
Values may be sent and summed in bfloat16 or wider, within the bound.
A program may use at most 64 MiB of HBM per device.

```python
import math
import jax
import jax.numpy as jnp
import numpy as np
from jax import lax

D = 2048
HEADS = 32
HEAD = 64
F = 512
FS = 512
TOPK = 6
SEQ_DEV = 16
TOKENS = 256
EXPERTS = 16
CAP = 12
DA = 2048
N_EP = 16
N_TP = 2


def shard_levels(stream_key, shape, split, smallest, top_value):
    gain, own = 1.0, jax.random.fold_in(stream_key, 6)
    for dim, parts in split:
        heights = jnp.exp(jax.random.uniform(jax.random.fold_in(own, dim), (parts,), jnp.float32, smallest / len(split), top_value / len(split)))
        gain = gain * jnp.repeat(heights, shape[dim] // parts).reshape([-1 if axis == dim else 1 for axis in range(len(shape))])
    return gain


def deal_out(own_key, own, number, rows, number_of, top, bound, slope):
    ranking = jax.random.permutation(own_key, number_of)
    packed, usual = portions_of(number_of, rows * top, bound, slope, True), portions_of(number_of, rows * top, bound, slope, False)
    places = jnp.arange(number_of)

    def named(lengths, offset_by):
        used = int((lengths > 0).sum())
        fixed = max(1, used // 4)
        shifted = fixed + (places - fixed + offset_by * (used - fixed)) % max(1, number_of - fixed)
        return jnp.zeros((number_of,), jnp.int32).at[ranking[jnp.where(places < fixed, places, shifted)]].set(jnp.asarray(lengths, jnp.int32))

    lengths = jnp.where(number % 4 == 0, named(packed, number // 4), named(usual, number - number // 4 - 1))
    mixed = jax.random.permutation(jax.random.fold_in(own, 3), number_of)
    giver, sink = mixed[0:number_of // 2 * 2:2], mixed[1:number_of // 2 * 2:2]
    slack = jnp.minimum(lengths[giver] - 1, bound - lengths[sink]) // 2
    slack = jnp.where((giver == ranking[0]) | (sink == ranking[0]) | (lengths[sink] == 0), 0, jnp.maximum(slack, 0))
    shifted = jax.random.randint(jax.random.fold_in(own, 4), (number_of // 2,), 0, 1 << 20) % (slack + 1)
    lengths = lengths.at[giver].add(-shifted).at[sink].add(shifted)
    items = jnp.searchsorted(jnp.cumsum(lengths), jnp.arange(rows * top), side="right").astype(jnp.int32)
    table = items.reshape(top, rows).T
    table = table[jax.random.permutation(jax.random.fold_in(own, 1), rows)]
    offset_by = jax.random.randint(jax.random.fold_in(own, 2), (rows, 1), 0, top)
    return jnp.take_along_axis(table, (jnp.arange(top)[None, :] + offset_by) % top, axis=1)


def portions_of(count, total, most, lean, full):
    portions = [(1 << 20) // math.isqrt(grade ** lean) + 1 for grade in range(1, count + 1)]
    largest = most if full else min(most, max(-(-total // count), total * portions[0] // sum(portions)))
    least = 1 if total - largest >= count - 1 else 0
    counts, surplus = [largest] + [least] * (count - 1), total - largest - least * (count - 1)
    while surplus > 0:
        candidates = [i for i in range(1, count) if counts[i] < largest] or [i for i in range(1, count) if counts[i] < most]
        mass, left = sum([portions[i] for i in candidates]), surplus
        for i in candidates:
            more = min(most - counts[i], max(1, left * portions[i] // mass), surplus)
            counts[i] = counts[i] + more
            surplus = surplus - more
    return np.array(counts)


def gaussian(rng, shape, width, bound, shards=(), kind=jnp.bfloat16):
    drawn = width * jax.random.normal(rng, shape, jnp.float32)
    if shards:
        drawn = drawn * shard_levels(rng, shape, shards, -0.22, 0.18)
    return jnp.clip(drawn, -bound, bound).astype(kind)


def setup_inputs(seed: int = 0) -> dict:
    splits = jax.random.split(jax.random.key(seed), 22)
    tokens = gaussian(splits[0], (TOKENS, D), 1.0, 6.0, ((0, 16), (1, 2)))
    state = gaussian(splits[1], (TOKENS, HEADS, HEAD * HEAD), 1.0, 6.0, ((0, 16), (1, 2)))
    mix_gain = jnp.clip(1.0 + 0.18 * jax.random.normal(splits[2], (D,), jnp.float32), 0.1, 1.9)
    w_recept = gaussian(splits[3], (D, DA), D ** -0.5, 0.125, ((0, 2), (1, 16)))
    w_key = gaussian(splits[4], (D, DA), D ** -0.5, 0.125, ((0, 2), (1, 16)))
    w_value = gaussian(splits[5], (D, DA), D ** -0.5, 0.125, ((0, 2), (1, 16)))
    w_decay = gaussian(splits[6], (D, DA), D ** -0.5, 0.125, ((0, 2), (1, 16)))
    w_rate = gaussian(splits[7], (D, DA), D ** -0.5, 0.125, ((0, 2), (1, 16)))
    decay_base = jnp.clip(-4.0 + 6.0 * jax.random.uniform(splits[8], (DA,), jnp.float32) ** shard_levels(splits[8], (DA,), ((0, 2),), -0.2, 0.2), -4.0, 2.0)
    rate_base = jnp.clip(jax.random.uniform(splits[9], (DA,), jnp.float32, -2.0, 2.0) * shard_levels(splits[9], (DA,), ((0, 2),), -0.4, 0.0), -2.0, 2.0)
    head_gain = jnp.clip(1.0 + 0.18 * jax.random.normal(splits[10], (DA,), jnp.float32), 0.1, 1.9)
    w_out = gaussian(splits[11], (DA, D), DA ** -0.5, 0.125, ((0, 2), (1, 16)))
    moe_gain = jnp.clip(1.0 + 0.18 * jax.random.normal(splits[12], (D,), jnp.float32), 0.1, 1.9)
    routes_keys = jax.random.split(jax.random.fold_in(splits[13], 1), TOKENS // SEQ_DEV)
    routes_turns = jax.random.permutation(jax.random.fold_in(splits[13], 3), TOKENS // SEQ_DEV)
    routes = jax.vmap(lambda own, number: deal_out(jax.random.fold_in(splits[13], 2), own, number, SEQ_DEV, EXPERTS, TOPK, CAP, 2))(routes_keys, routes_turns).reshape((TOKENS, TOPK))
    route_weight = jnp.clip(jnp.exp(math.log(1.0) - 2.3025851 * jax.random.uniform(splits[14], (TOKENS, TOPK), jnp.float32) ** shard_levels(splits[14], (TOKENS, TOPK), ((0, 16),), -0.2, 0.2)), 0.1, 1.0)
    expert_gate = gaussian(splits[15], (EXPERTS, D, F), D ** -0.5, 0.125, ((0, 16), (2, 2)))
    expert_up = gaussian(splits[16], (EXPERTS, D, F), D ** -0.5, 0.125, ((0, 16), (2, 2)))
    expert_down = gaussian(splits[17], (EXPERTS, F, D), F ** -0.5, 0.25, ((0, 16), (1, 2)))
    shared_gate = gaussian(splits[18], (D, FS), D ** -0.5, 0.125, ((1, 2),))
    shared_up = gaussian(splits[19], (D, FS), D ** -0.5, 0.125, ((1, 2),))
    shared_down = gaussian(splits[20], (FS, D), FS ** -0.5, 0.25, ((0, 2),))
    return dict(tokens=tokens, state=state, mix_gain=mix_gain, w_recept=w_recept, w_key=w_key, w_value=w_value, w_decay=w_decay, w_rate=w_rate, decay_base=decay_base, rate_base=rate_base, head_gain=head_gain, w_out=w_out, moe_gain=moe_gain, routes=routes, route_weight=route_weight, expert_gate=expert_gate, expert_up=expert_up, expert_down=expert_down, shared_gate=shared_gate, shared_up=shared_up, shared_down=shared_down)


RMS_EPS = 1e-06
GN_EPS = 0.00064
KEY_EPS = 1e-06
ROUTED_SCALE = 2.5

def row_norm(row_vals, gain_vals):
    row32 = row_vals.astype(jnp.float32)
    factor = lax.rsqrt(lax.optimization_barrier(jnp.mean(row32 * row32, axis=-1, keepdims=True)) + RMS_EPS)
    return (row32 * factor * gain_vals).astype(jnp.bfloat16)

def quarter_dot(left_vals, weight):
    row_count = left_vals.shape[0]
    part_len = left_vals.shape[1] // N_TP
    left_parts = left_vals.reshape(row_count, N_TP, part_len).astype(jnp.float32)
    weight_parts = weight.reshape(N_TP, part_len, weight.shape[1]).astype(jnp.float32)
    partial_value = jnp.einsum('rqk,qkm->rqm', left_parts, weight_parts)
    rounded = lax.optimization_barrier(partial_value.astype(jnp.bfloat16))
    return lax.optimization_barrier(jnp.sum(rounded.astype(jnp.float32), axis=1))

def mixer_rows(state_rows, projected, decay_base, rate_base, head_gain):
    seq_count = projected.shape[0]
    head_count = projected.shape[2] // HEAD

    def per_head(column):
        return projected[:, column, :].reshape(seq_count, head_count, HEAD)
    receptance = per_head(0)
    key_vec = per_head(1)
    value_vec = per_head(2)
    decay_pre = (projected[:, 3, :] + decay_base).reshape(seq_count, head_count, HEAD)
    rate_pre = (projected[:, 4, :] + rate_base).reshape(seq_count, head_count, HEAD)
    decay_rate = jnp.exp(-jnp.exp(-jax.nn.softplus(-decay_pre) - 0.5))
    in_rate = jax.nn.sigmoid(rate_pre)
    unit_key = key_vec * lax.rsqrt(lax.optimization_barrier(jnp.sum(key_vec * key_vec, axis=-1, keepdims=True)) + KEY_EPS)
    carried = state_rows.astype(jnp.float32).reshape(seq_count, head_count, HEAD, HEAD)
    removed = jnp.einsum('nhvk,nhk->nhv', carried, unit_key)
    updated = carried * decay_rate[:, :, None, :] - removed[:, :, :, None] * (unit_key * in_rate)[:, :, None, :] + value_vec[:, :, :, None] * (key_vec * in_rate)[:, :, None, :]
    readout = jnp.einsum('nhvk,nhk->nhv', updated, receptance)
    centre = lax.optimization_barrier(jnp.mean(readout, axis=-1, keepdims=True))
    spread = lax.optimization_barrier(jnp.mean(jnp.square(readout - centre), axis=-1, keepdims=True))
    normed = (readout - centre) * lax.rsqrt(spread + GN_EPS)
    return (normed.reshape(seq_count, head_count * HEAD) * head_gain).astype(jnp.bfloat16)

def reference(tokens, state, mix_gain, w_recept, w_key, w_value, w_decay, w_rate, decay_base, rate_base, head_gain, w_out, moe_gain, routes, route_weight, expert_gate, expert_up, expert_down, shared_gate, shared_up, shared_down):
    normed = row_norm(tokens, mix_gain)
    projected = jnp.stack([quarter_dot(normed, weight) for weight in (w_recept, w_key, w_value, w_decay, w_rate)], axis=1)

    def mix_group(item):
        return mixer_rows(item[0], item[1], decay_base, rate_base, head_gain)
    mixed = lax.map(mix_group, (state.reshape(N_EP, SEQ_DEV, HEADS, HEAD * HEAD), projected.reshape(N_EP, SEQ_DEV, 5, HEADS * HEAD)))
    mixed = mixed.reshape(TOKENS, HEADS * HEAD)
    attended = quarter_dot(mixed, w_out)
    resid = (tokens.astype(jnp.float32) + attended).astype(jnp.bfloat16)
    normed_two = row_norm(resid, moe_gain)
    shared_hidden = (jax.nn.silu(jnp.dot(normed_two, shared_gate, preferred_element_type=jnp.float32)) * jnp.dot(normed_two, shared_up, preferred_element_type=jnp.float32)).astype(jnp.bfloat16)
    shared_out = quarter_dot(shared_hidden, shared_down)
    per_group = SEQ_DEV * TOPK
    grouped = routes.reshape(N_EP, per_group)
    position = jnp.arange(per_group, dtype=jnp.int32)
    earlier = (grouped[:, :, None] == grouped[:, None, :]) & (position[None, None, :] < position[None, :, None])
    rank_in = lax.optimization_barrier(jnp.sum(earlier.astype(jnp.int32), axis=2))
    group_ids = jnp.arange(N_EP, dtype=jnp.int32)[:, None]
    flat_slot = ((grouped * N_EP + group_ids) * CAP + rank_in).reshape(-1).astype(jnp.int32)
    owner_token = (jnp.arange(TOKENS, dtype=jnp.int32)[:, None] + jnp.zeros((1, TOPK), jnp.int32)).reshape(-1)
    slot_total = EXPERTS * N_EP * CAP
    table = jnp.zeros((slot_total,), jnp.int32).at[flat_slot].set(owner_token)
    live = jnp.zeros((slot_total,), jnp.float32).at[flat_slot].set(1.0)

    def run_expert(item):
        row_index, live_rows, gate_w, up_w, down_w = item
        chosen_rows = jnp.take(normed_two, row_index, axis=0)
        gate_val = jnp.dot(chosen_rows, gate_w, preferred_element_type=jnp.float32)
        up_val = jnp.dot(chosen_rows, up_w, preferred_element_type=jnp.float32)
        hidden = (jax.nn.silu(gate_val) * up_val).astype(jnp.bfloat16)
        return (quarter_dot(hidden, down_w) * live_rows[:, None]).astype(jnp.bfloat16)
    expert_rows = lax.map(run_expert, (table.reshape(EXPERTS, N_EP * CAP), live.reshape(EXPERTS, N_EP * CAP), expert_gate, expert_up, expert_down))
    picked = jnp.take(expert_rows.reshape(slot_total, D), flat_slot, axis=0)
    picked = picked.astype(jnp.float32).reshape(TOKENS, TOPK, D)
    share = route_weight / lax.optimization_barrier(jnp.sum(route_weight, axis=1, keepdims=True)) * ROUTED_SCALE
    routed = lax.optimization_barrier(jnp.sum(share[:, :, None] * picked, axis=1))
    return (resid.astype(jnp.float32) + routed + shared_out).astype(jnp.bfloat16)
```

```python
import functools
import math

import jax
import jax.numpy as jnp
from jax import lax
from jax.experimental import pallas as pl
from jax.experimental.pallas import tpu as pltpu
from jax.sharding import PartitionSpec as P

HEAD = 64


RMS_EPS = 1e-06
GN_EPS = 0.00064
KEY_EPS = 1e-06
ROUTED_SCALE = 2.5
EXP_HALF = math.exp(-0.5)


def for_sending(array):
    return jax.tree.map(lambda a: a.astype(jnp.bfloat16) if a.dtype == jnp.float32 else a, array)


def mixer_rows(state_rows, projected, decay_base, rate_base, head_gain):
    seq_count = projected.shape[0]
    head_count = projected.shape[2] // HEAD

    def per_head(column):
        return projected[:, column, :].reshape(seq_count, head_count, HEAD)

    receptance = per_head(0)
    key_vec = per_head(1)
    value_vec = per_head(2)
    decay_pre = (projected[:, 3, :] + decay_base).reshape(seq_count, head_count, HEAD)
    rate_pre = (projected[:, 4, :] + rate_base).reshape(seq_count, head_count, HEAD)
    decay_rate = jnp.exp(-jnp.exp(-jax.nn.softplus(-decay_pre) - 0.5))
    in_rate = jax.nn.sigmoid(rate_pre)
    unit_key = key_vec * lax.rsqrt(jnp.sum(key_vec * key_vec, axis=-1, keepdims=True) + KEY_EPS)
    carried = state_rows.astype(jnp.float32).reshape(seq_count, head_count, HEAD, HEAD)
    removed = jnp.einsum("nhvk,nhk->nhv", carried, unit_key)
    updated = (
        carried * decay_rate[:, :, None, :]
        - removed[:, :, :, None] * (unit_key * in_rate)[:, :, None, :]
        + value_vec[:, :, :, None] * (key_vec * in_rate)[:, :, None, :]
    )
    readout = jnp.einsum("nhvk,nhk->nhv", updated, receptance)
    centre = jnp.mean(readout, axis=-1, keepdims=True)
    spread = jnp.mean(jnp.square(readout - centre), axis=-1, keepdims=True)
    normed = (readout - centre) * lax.rsqrt(spread + GN_EPS)
    return (normed.reshape(seq_count, head_count * HEAD) * head_gain).astype(jnp.bfloat16)


def quarter_sums(partial_value):
    return jax.tree.map(
        lambda part: part.astype(jnp.float32),
        lax.psum_scatter(for_sending(partial_value), "tp", scatter_dimension=2, tiled=True),
    )


def project_split(part_rows, weight_cols):
    inner_len = weight_cols.shape[0]
    role_count = weight_cols.shape[1]
    col_width = weight_cols.shape[2]
    flat_weight = weight_cols.reshape(inner_len, role_count * col_width)
    block_rows = lax.all_gather(part_rows, "ep", axis=0, tiled=True)
    product = jnp.dot(block_rows, flat_weight, preferred_element_type=jnp.float32)
    gathered = product.astype(jnp.bfloat16).reshape(block_rows.shape[0], role_count, col_width)
    owned = lax.all_to_all(gathered, "ep", split_axis=0, concat_axis=2, tiled=True)
    return quarter_sums(owned.astype(jnp.float32))


def body(
    tokens,
    state,
    mix_gain,
    w_recept,
    w_key,
    w_value,
    w_decay,
    w_rate,
    decay_base,
    rate_base,
    head_gain,
    w_out,
    moe_gain,
    routes,
    route_weight,
    expert_gate,
    expert_up,
    expert_down,
    shared_gate,
    shared_up,
    shared_down,
):
    seq_count = tokens.shape[0]
    quarter = tokens.shape[1]
    width_all = quarter * lax.axis_size("tp")
    ep_count = lax.axis_size("ep")
    topk_count = routes.shape[1]
    capacity = min(seq_count, max(2, 2 * seq_count * topk_count // ep_count))
    tokens32 = tokens.astype(jnp.float32)
    square_sum = lax.psum(jnp.sum(tokens32 * tokens32, axis=1), "tp")
    factor = lax.rsqrt(square_sum / width_all + RMS_EPS)
    normed = (tokens32 * factor[:, None] * mix_gain).astype(jnp.bfloat16)
    stacked = jnp.stack((w_recept, w_key, w_value, w_decay, w_rate), axis=1)
    projected = project_split(normed, stacked)
    mixed = mixer_rows(state, projected, decay_base, rate_base, head_gain)
    attended = project_split(mixed, w_out[:, None, :])[:, 0, :]
    resid = (tokens32 + attended).astype(jnp.bfloat16)
    full_resid = lax.all_gather(resid, "tp", axis=1, tiled=True).astype(jnp.float32)
    moe_factor = lax.rsqrt(jnp.mean(full_resid * full_resid, axis=1, keepdims=True) + RMS_EPS)
    normed_two = (full_resid * moe_factor * moe_gain).astype(jnp.bfloat16)
    shared_hidden = (
        jax.nn.silu(jnp.dot(normed_two, shared_gate, preferred_element_type=jnp.float32))
        * jnp.dot(normed_two, shared_up, preferred_element_type=jnp.float32)
    ).astype(jnp.bfloat16)
    shared_part = jnp.dot(shared_hidden, shared_down, preferred_element_type=jnp.float32)
    entry_count = seq_count * topk_count
    flat_routes = routes.reshape(entry_count)
    position = jnp.arange(entry_count, dtype=jnp.int32)
    earlier = (flat_routes[:, None] == flat_routes[None, :]) & (
        position[None, :] < position[:, None]
    )
    rank_in = jnp.sum(earlier.astype(jnp.int32), axis=1)
    local_slot = flat_routes * capacity + rank_in
    slot_count = ep_count * capacity
    slot_ids = jnp.arange(slot_count, dtype=jnp.int32)
    matches = (slot_ids[:, None] == local_slot[None, :]).astype(jnp.float32)
    dispatch_map = jnp.sum(matches.reshape(slot_count, seq_count, topk_count), axis=2).astype(
        jnp.bfloat16
    )
    outgoing = jnp.dot(dispatch_map, normed_two, preferred_element_type=jnp.float32)
    outgoing = outgoing.astype(jnp.bfloat16).reshape(ep_count, capacity, width_all)
    arrived = lax.all_to_all(outgoing, "ep", split_axis=0, concat_axis=0, tiled=True)
    expert_in = arrived.reshape(slot_count, width_all)
    hidden = (
        jax.nn.silu(jnp.dot(expert_in, expert_gate[0], preferred_element_type=jnp.float32))
        * jnp.dot(expert_in, expert_up[0], preferred_element_type=jnp.float32)
    ).astype(jnp.bfloat16)
    expert_part = jnp.dot(hidden, expert_down[0], preferred_element_type=jnp.float32)
    routed_sum, shared_sum = quarter_sums((expert_part[:, None, :], shared_part[:, None, :]))
    expert_out = routed_sum[:, 0, :].astype(jnp.bfloat16).reshape(ep_count, capacity, quarter)
    came_back = lax.all_to_all(expert_out, "ep", split_axis=0, concat_axis=0, tiled=True).reshape(
        slot_count, quarter
    )
    picked = (
        jnp.take(came_back, local_slot, axis=0)
        .astype(jnp.float32)
        .reshape(seq_count, topk_count, quarter)
    )
    share = route_weight / jnp.sum(route_weight, axis=1, keepdims=True) * ROUTED_SCALE
    routed = jnp.sum(share[:, :, None] * picked, axis=1)
    return (resid.astype(jnp.float32) + routed + shared_sum[:, 0, :]).astype(jnp.bfloat16)


def fits_fused(ep_count, tp_count, col_width, head_rows, quarter):
    return (
        tp_count == 2
        and ep_count >= 8
        and ep_count & (ep_count - 1) == 0
        and ep_count <= HEAD
        and col_width % 128 == 0
        and quarter * tp_count == ep_count * col_width
        and head_rows % 16 == 0
    )


def fused_kernel(
    dims,
    tokens,
    state,
    mix_gain,
    w_recept,
    w_key,
    w_value,
    w_decay,
    w_rate,
    decay_base,
    rate_base,
    head_gain,
    w_out,
    moe_gain,
    routes,
    route_weight,
    expert_gate,
    expert_up,
    expert_down,
    shared_gate,
    shared_up,
    shared_down,
    out,
    tok_buf,
    sq_buf,
    prod_buf,
    prod_in,
    mix_buf,
    att_f,
    att_out,
    att_in,
    res_buf,
    y_buf,
    r_in,
    s_buf,
    z_in,
    head_buf,
    ones_map,
    v_state,
    v_w,
    v_wout,
    v_gate,
    v_up,
    v_down,
    v_sgate,
    v_sup,
    v_sdown,
    load_sem,
    swap_send,
    swap_recv,
    tok_send,
    tok_recv,
    sq_send,
    sq_recv,
    prod_send,
    prod_recv,
    mix_send,
    mix_recv,
    att_send,
    att_recv,
    res_send,
    res_recv,
    r_send,
    r_recv,
    s_send,
    s_recv,
):
    ep_n, tp_n, seq, quarter, colw, width = dims
    f32, bf16 = jnp.float32, jnp.bfloat16
    chips = ep_n // 2
    group = chips // tp_n
    planes = chips // 2
    cols = 2 * colw
    heads = quarter // HEAD
    rows = seq * heads
    pair_cols = cols // 128
    total_rows = chips * seq
    me = lax.axis_index("ep")
    my_t = lax.axis_index("tp")
    core = lax.rem(me, 2)
    chip = me // 2
    sister = chip * 2 + 1 - core
    plane, side = chip // 2, lax.rem(chip, 2)
    owner, slot = chip // group, lax.rem(chip, group)

    def remote(src, dst, send, recv, ep_to, tp_to):
        return pltpu.make_async_remote_copy(
            src_ref=src,
            dst_ref=dst,
            send_sem=send,
            recv_sem=recv,
            device_id={"ep": ep_to, "tp": tp_to},
            device_id_type=pl.DeviceIdType.MESH,
        )

    def at(z, x):
        return (z * 2 + x) * 2 + core

    def flip(z, k):
        bit = 1
        res = z
        while bit <= k:
            if k & bit:
                res = res + bit * (1 - 2 * lax.rem(z // bit, 2))
            bit *= 2
        return res

    loads = []

    def load(src, dst):
        copy = pltpu.make_async_copy(src, dst, load_sem.at[len(loads)])
        copy.start()
        loads.append(copy)
        return copy

    def w_slot(p):
        return v_w.at[:, pl.ds(pl.multiple_of(p * cols + core * colw, 128), colw)]

    own_expert = pl.ds(core, 1)
    w_list = (w_recept, w_key, w_value, w_decay, w_rate)
    wout_slot = v_wout.at[:, pl.ds(pl.multiple_of(core * colw, 128), colw)]
    ld_tok = load(tokens, tok_buf.at[chip, :, :quarter])
    ld_w = [load(w, w_slot(p)) for p, w in enumerate(w_list)]
    ld_state = load(state, v_state)
    ld_wout = load(w_out, wout_slot)
    ld_shared = [
        load(a, b) for a, b in ((shared_gate, v_sgate), (shared_up, v_sup), (shared_down, v_sdown))
    ]
    ld_expert = [
        load(a, b.at[own_expert])
        for a, b in ((expert_gate, v_gate), (expert_up, v_up), (expert_down, v_down))
    ]

    barrier = pltpu.get_barrier_semaphore()

    def greet_one(e_to, t_to):
        pl.semaphore_signal(
            barrier,
            inc=1,
            device_id={"ep": e_to, "tp": t_to},
            device_id_type=pl.DeviceIdType.MESH,
        )

    def greet(k, carry):
        greet_one(lax.rem(chip + k // tp_n, chips) * 2 + core, lax.rem(my_t + lax.rem(k, tp_n), tp_n))
        return carry

    lax.fori_loop(1, chips * tp_n, greet, 0)
    greet_one(sister, my_t)

    weight = route_weight[...]
    share = weight / jnp.sum(weight, axis=0, keepdims=True) * ROUTED_SCALE
    experts = lax.broadcasted_iota(jnp.int32, (128, seq), 0) % HEAD
    dense = jnp.zeros((128, seq), f32)
    for k in range(routes.shape[0]):
        dense += jnp.where(routes[k : k + 1, :] == experts, share[k : k + 1, :], 0.0)
    dense = dense.T
    lanes = lax.broadcasted_iota(jnp.int32, (seq, 128), 1)
    high = dense.astype(bf16).astype(f32)
    tok_buf[chip, :, quarter:] = jnp.where(lanes < HEAD, high, dense - high).astype(bf16)

    big_rows = ones_map.shape[0]
    row_id = lax.broadcasted_iota(jnp.int32, (big_rows, 128), 0)
    lane_id = lax.broadcasted_iota(jnp.int32, (big_rows, 128), 1)
    ones_map[...] = jnp.where(row_id // HEAD == lane_id % HEAD, 1.0, 0.0).astype(bf16)

    ld_tok.wait()
    own_tok = tok_buf[chip, :, :quarter].astype(f32)
    sq_buf[my_t] = jnp.broadcast_to(jnp.sum(own_tok * own_tok, axis=1, keepdims=True), (seq, 128))

    pl.semaphore_wait(barrier, chips * tp_n)

    far_first = list(range(planes - 1, 0, -1))

    def gather_start(buf, send, recv):
        def put(i, to):
            remote(buf.at[chip], buf.at[chip], send.at[i], recv.at[chip], to, my_t).start()

        for k in far_first:
            put(k, at(flip(plane, k), side))
        put(0, at(plane, 1 - side))

    def gather_finish(buf, send, recv):
        def arrived(src):
            remote(buf.at[src], buf.at[src], send.at[0], recv.at[src], me, my_t).wait_recv()

        for k in far_first:
            src = flip(plane, k) * 2 + side
            arrived(src)
            remote(
                buf.at[src], buf.at[src], send.at[planes - 1 + k], recv.at[src], at(plane, 1 - side), my_t
            ).start()
        for k in [0] + far_first:
            arrived(flip(plane, k) * 2 + 1 - side)

    def drain(count, make):
        def step(k, carry):
            make(k).wait_send()
            return carry

        lax.fori_loop(0, count, step, 0)

    def gather_drain(buf, send, recv):
        drain(
            2 * planes - 1,
            lambda k: remote(buf.at[chip], buf.at[chip], send.at[k], recv.at[chip], sister, my_t),
        )

    gather_start(tok_buf, tok_send, tok_recv)
    sq_copy = remote(sq_buf.at[my_t], sq_buf.at[my_t], sq_send, sq_recv, me, 1 - my_t)
    sq_copy.start()

    def swap(i, src, dst):
        return remote(src, dst, swap_send.at[i], swap_recv.at[i], sister, my_t)

    swap_w = [swap(p, w, w_slot(p)) for p, w in enumerate(w_list)]
    swap_late = [swap(5, w_out, wout_slot)] + [
        swap(6 + i, a, b.at[own_expert])
        for i, (a, b) in enumerate(((expert_gate, v_gate), (expert_up, v_up), (expert_down, v_down)))
    ]
    for copy in swap_w:
        copy.start()

    for copy in ld_w:
        copy.wait()
    for copy in swap_w:
        copy.wait_recv()
    gather_finish(tok_buf, tok_send, tok_recv)
    tok_all = tok_buf[:, :, :quarter].astype(f32).reshape(total_rows, quarter)
    scaled = (tok_all * mix_gain[...]).astype(bf16)
    product = jnp.dot(scaled, v_w[...], preferred_element_type=f32)
    prod_buf[...] = product.astype(bf16).reshape(chips, seq, 5 * cols)

    def prod_copy(k, to):
        return remote(
            prod_buf.at[to],
            prod_in.at[my_t, slot],
            prod_send.at[k],
            prod_recv.at[my_t, slot],
            to * 2 + core,
            owner,
        )

    for k in range(chips - 1, 0, -1):
        prod_copy(k, flip(chip, k)).start()

    @pl.when(owner == my_t)
    def _():
        prod_in[my_t, slot] = prod_buf[chip]

    @pl.when(owner != my_t)
    def _():
        prod_copy(0, chip).start()

    for copy in swap_late:
        copy.start()
    gather_drain(tok_buf, tok_send, tok_recv)
    for copy in swap_w:
        copy.wait_send()
    sq_copy.wait_send()
    remote(sq_buf.at[1 - my_t], sq_buf.at[1 - my_t], sq_send, sq_recv, me, my_t).wait_recv()
    factor = lax.rsqrt((sq_buf[0] + sq_buf[1])[:, :1] / width + RMS_EPS)
    ld_state.wait()

    def recv_prod(k, carry):
        src_t, src_slot = k // group, lax.rem(k, group)
        mine = (src_t == my_t) & (my_t * group + src_slot == chip)

        @pl.when(jnp.logical_not(mine))
        def _():
            remote(
                prod_buf.at[0],
                prod_in.at[src_t, src_slot],
                prod_send.at[0],
                prod_recv.at[src_t, src_slot],
                me,
                my_t,
            ).wait_recv()

        return carry

    lax.fori_loop(0, tp_n * group, recv_prod, 0)

    low_half = lax.broadcasted_iota(jnp.int32, (seq, 128), 1) < HEAD
    for g in range(group):
        total = prod_in[0, g].astype(f32)
        for t in range(1, tp_n):
            total += prod_in[t, g].astype(f32)
        total = total * factor
        for p in range(5):
            for i in range(pair_cols):
                pair = g * pair_cols + i
                val = total[:, p * cols + i * 128 : p * cols + (i + 1) * 128]
                if p == 3:
                    val = val + decay_base[:, pair * 128 : (pair + 1) * 128]
                if p == 4:
                    val = val + rate_base[:, pair * 128 : (pair + 1) * 128]
                turned = pltpu.roll(val, HEAD, 1)
                head_buf[p, pl.ds(2 * pair, seq, stride=heads), :] = jnp.where(low_half, val, turned)
                head_buf[p, pl.ds(2 * pair + 1, seq, stride=heads), :] = jnp.where(
                    low_half, turned, val
                )

    def half_sum(x):
        return 0.5 * jnp.sum(x, axis=1, keepdims=True)

    recept, key, value = head_buf[0], head_buf[1], head_buf[2]
    decay = jnp.exp(-jax.nn.sigmoid(head_buf[3]) * EXP_HALF)
    rate = jax.nn.sigmoid(head_buf[4])
    unit = key * lax.rsqrt(half_sum(key * key) + KEY_EPS)
    rated = rate * recept
    removed_by = half_sum(unit * rated)
    added_by = half_sum(key * rated)
    left = (decay * recept).astype(bf16)
    right = unit.astype(bf16)
    step = 512
    left_wide = jnp.concatenate([left] * (step // 128), axis=1)
    right_wide = jnp.concatenate([right] * (step // 128), axis=1)
    read_left = jnp.zeros((rows, 128), f32)
    read_right = jnp.zeros((rows, 128), f32)
    for c in range(HEAD * HEAD // step):
        block = v_state[:, c * step : (c + 1) * step]
        ones = ones_map[c * step : (c + 1) * step, :]
        read_left += jnp.dot(block * left_wide, ones, preferred_element_type=f32)
        read_right += jnp.dot(block * right_wide, ones, preferred_element_type=f32)
    readout = read_left - read_right * removed_by + value * added_by
    centred = readout - half_sum(readout) / HEAD
    spread = half_sum(centred * centred) / HEAD
    head_buf[0] = centred * lax.rsqrt(spread + GN_EPS)
    for pair in range(heads // 2):
        even = head_buf[0, pl.ds(2 * pair, seq, stride=heads), :]
        odd = head_buf[0, pl.ds(2 * pair + 1, seq, stride=heads), :]
        span = slice(pair * 128, (pair + 1) * 128)
        mix_buf[chip, :, span] = (jnp.where(low_half, even, odd) * head_gain[:, span]).astype(bf16)

    gather_start(mix_buf, mix_send, mix_recv)
    drain(chips - 1, lambda k: prod_copy(k + 1, chip))

    @pl.when(owner != my_t)
    def _():
        prod_copy(0, chip).wait_send()

    ld_wout.wait()
    swap_late[0].wait_recv()
    gather_finish(mix_buf, mix_send, mix_recv)
    attended = jnp.dot(
        mix_buf[...].reshape(total_rows, quarter), v_wout[...], preferred_element_type=f32
    )
    token = tok_buf[:, :, pl.ds(pl.multiple_of(slot * cols, 128), cols)].astype(f32)
    attended += jnp.where(owner == my_t, token.reshape(total_rows, cols), 0.0)
    half_rows = total_rows // tp_n
    att_f[...] = attended.reshape(tp_n, half_rows, cols)
    att_out[...] = att_f[1 - my_t].astype(bf16)
    att_copy = remote(att_out, att_in, att_send, att_recv, me, 1 - my_t)
    att_copy.start()
    gather_drain(mix_buf, mix_send, mix_recv)
    att_copy.wait_recv()
    res_buf[chip, my_t] = (att_f[my_t] + att_in[...].astype(f32)).astype(bf16)

    def res_copy(i, c, e_to, t_to):
        return remote(
            res_buf.at[c, my_t], res_buf.at[c, my_t], res_send.at[i], res_recv.at[c, my_t], e_to, t_to
        )

    def res_arrived(c, t):
        remote(
            res_buf.at[c, t], res_buf.at[c, t], res_send.at[0], res_recv.at[c, t], me, my_t
        ).wait_recv()

    def res_spread(k):
        c = flip(plane, k) * 2 + side
        res_copy(planes + 3 * k, c, at(plane, 1 - side), 1 - my_t).start()
        res_copy(planes + 3 * k + 1, c, at(plane, 1 - side), my_t).start()
        res_copy(planes + 3 * k + 2, c, at(plane, side), 1 - my_t).start()

    for k in far_first:
        res_copy(k, chip, at(flip(plane, k), side), my_t).start()
    res_spread(0)
    for copy in ld_shared + ld_expert:
        copy.wait()
    for copy in swap_late[1:]:
        copy.wait_recv()
    for k in far_first:
        res_arrived(flip(plane, k) * 2 + side, my_t)
        res_spread(k)

    own_rows = pl.ds(pl.multiple_of(lax.rem(chip, group) * seq, seq), seq)
    own_half = chip // group
    square_sum = jnp.zeros((total_rows, 1), f32)
    sums = [jnp.zeros((total_rows, v_gate.shape[2]), f32) for _ in range(4)]
    own_sums = [jnp.zeros((seq, v_sgate.shape[1]), f32) for _ in range(2)]
    for x in (0, 1):
        for k in [0] + far_first:
            c = flip(plane, k) * 2 + (1 - side if x else side)
            if x:
                res_arrived(c, my_t)
            res_arrived(c, 1 - my_t)
            span = pl.ds(pl.multiple_of(c * cols, 128), cols)
            part = res_buf[c].astype(f32).reshape(total_rows, cols)
            square_sum += jnp.sum(part * part, axis=1, keepdims=True)
            gained = (part * moe_gain[:, span]).astype(bf16)
            for j in range(2):
                sums[j] += jnp.dot(gained, v_gate[j, span, :], preferred_element_type=f32)
                sums[2 + j] += jnp.dot(gained, v_up[j, span, :], preferred_element_type=f32)
            own = res_buf[c, own_half, own_rows, :].astype(f32)
            own = (own * moe_gain[:, span]).astype(bf16)
            own_sums[0] += jnp.dot(own, v_sgate[span, :], preferred_element_type=f32)
            own_sums[1] += jnp.dot(own, v_sup[span, :], preferred_element_type=f32)

    def gated(g, u):
        return g * jax.nn.sigmoid(g) * u

    factor = lax.rsqrt(square_sum / width + RMS_EPS)
    tail = tok_buf[:, :, quarter:].astype(f32).reshape(total_rows, 128)
    lanes = lax.broadcasted_iota(jnp.int32, (total_rows, 128), 1) % HEAD
    hidden = []
    for j in range(2):
        mine = jnp.sum(jnp.where(lanes == chip * 2 + j, tail, 0.0), axis=1, keepdims=True)
        hidden.append((gated(sums[j] * factor, sums[2 + j] * factor) * mine).astype(bf16))
    hidden = jnp.concatenate(hidden, axis=1)
    own_res = jnp.zeros((seq, 1), f32)
    for c in range(chips):
        part = res_buf[c, own_half, own_rows, :].astype(f32)
        own_res += jnp.sum(part * part, axis=1, keepdims=True)
    own_factor = lax.rsqrt(own_res / width + RMS_EPS)
    shared_hidden = gated(own_sums[0] * own_factor, own_sums[1] * own_factor).astype(bf16)
    down = v_down[...].reshape(2 * v_down.shape[1], width)
    for t in range(tp_n):
        span = slice(t * quarter, (t + 1) * quarter)
        routed = jnp.dot(hidden, down[:, span], preferred_element_type=f32)
        y_buf[t] = routed.astype(bf16).reshape(chips, seq, quarter)
        shared_part = jnp.dot(shared_hidden, v_sdown[:, span], preferred_element_type=f32)
        y_buf[t, chip] = (y_buf[t, chip].astype(f32) + shared_part).astype(bf16)

    turns = ((1, 1), (1, 0), (0, 1))

    def ret_copy(k, j):
        dx, dy = turns[j]
        z = flip(plane, k)
        x_to = 1 - side if dx else side
        t_to = 1 - my_t if dy else my_t
        return remote(
            y_buf.at[t_to, z * 2 + x_to],
            r_in.at[j, z],
            r_send.at[3 * k + j],
            r_recv.at[j, z],
            at(plane, x_to),
            t_to,
        )

    def sum_copy(k):
        z = flip(plane, k)
        return remote(s_buf.at[z], z_in.at[plane], s_send.at[k], s_recv.at[plane], at(z, side), my_t)

    order = far_first + [0]
    for k in order:
        for j in range(3):
            ret_copy(k, j).start()
    total = jnp.zeros((seq, quarter), f32)
    for k in order:
        z = flip(plane, k)
        total = y_buf[my_t, z * 2 + side].astype(f32)
        for j in range(3):
            ret_copy(k, j).wait_recv()
            total += r_in[j, z].astype(f32)
        if k:
            s_buf[z] = total.astype(bf16)
            sum_copy(k).start()
    for g in range(group):
        part = res_buf[my_t * group + g, own_half, own_rows, :].astype(f32)
        s_own = total[:, g * cols : (g + 1) * cols] + part
        att_f[0, pl.ds(g * seq, seq), :] = s_own
    for k in range(1, planes):
        res_copy(k, chip, me, my_t).wait_send()
    drain(3 * planes, lambda k: res_copy(planes + k, chip, me, my_t))
    att_copy.wait_send()
    for copy in swap_late:
        copy.wait_send()
    for k in order:
        for j in range(3):
            ret_copy(k, j).wait_send()
    for k in far_first:
        z = flip(plane, k)
        remote(s_buf.at[z], z_in.at[z], s_send.at[k], s_recv.at[z], me, my_t).wait_recv()
    for g in range(group):
        span = slice(g * cols, (g + 1) * cols)
        res = att_f[0, pl.ds(g * seq, seq), :]
        for k in far_first:
            res += z_in[flip(plane, k), :, span].astype(f32)
        out[:, span] = res.astype(bf16)
    for k in far_first:
        sum_copy(k).wait_send()


def fused_body(*args):
    args = list(args)
    tokens, state, w_recept = args[0], args[1], args[3]
    seq, quarter = tokens.shape
    ep_n, tp_n = lax.axis_size("ep"), lax.axis_size("tp")
    colw = w_recept.shape[1]
    width = quarter * tp_n
    heads = state.shape[1]
    chips = ep_n // 2
    group, planes, cols = chips // tp_n, chips // 2, 2 * colw
    args[1] = state.reshape(seq * heads, state.shape[2])
    for i in (2, 8, 9, 10, 12):
        args[i] = args[i].reshape(1, -1)
    for i in (13, 14):
        args[i] = args[i].T
    hidden, shared = args[15].shape[2], args[18].shape[1]
    bf16, f32, dma = jnp.bfloat16, jnp.float32, pltpu.SemaphoreType.DMA
    vmem = {2, 8, 9, 10, 12, 13, 14}
    specs = [
        pl.BlockSpec(memory_space=pltpu.VMEM if i in vmem else pl.ANY) for i in range(len(args))
    ]
    half_rows = chips * seq // tp_n
    scratch = [
        pltpu.VMEM((chips, seq, quarter + 128), bf16),
        pltpu.VMEM((tp_n, seq, 128), f32),
        pltpu.VMEM((chips, seq, 5 * cols), bf16),
        pltpu.VMEM((tp_n, group, seq, 5 * cols), bf16),
        pltpu.VMEM((chips, seq, quarter), bf16),
        pltpu.VMEM((tp_n, half_rows, cols), f32),
        pltpu.VMEM((half_rows, cols), bf16),
        pltpu.VMEM((half_rows, cols), bf16),
        pltpu.VMEM((chips, tp_n, half_rows, cols), bf16),
        pltpu.VMEM((tp_n, chips, seq, quarter), bf16),
        pltpu.VMEM((3, planes, seq, quarter), bf16),
        pltpu.VMEM((planes, seq, quarter), bf16),
        pltpu.VMEM((planes, seq, quarter), bf16),
        pltpu.VMEM((5, seq * heads, 128), f32),
        pltpu.VMEM((HEAD * HEAD, 128), bf16),
        pltpu.VMEM(args[1].shape, bf16),
        pltpu.VMEM((quarter, 5 * cols), bf16),
        pltpu.VMEM((quarter, cols), bf16),
        pltpu.VMEM((2, width, hidden), bf16),
        pltpu.VMEM((2, width, hidden), bf16),
        pltpu.VMEM((2, hidden, width), bf16),
        pltpu.VMEM((width, shared), bf16),
        pltpu.VMEM((width, shared), bf16),
        pltpu.VMEM((shared, width), bf16),
        dma((16,)),
        dma((9,)),
        dma((9,)),
        dma((2 * planes - 1,)),
        dma((chips,)),
        dma(()),
        dma(()),
        dma((chips,)),
        dma((tp_n, group)),
        dma((2 * planes - 1,)),
        dma((chips,)),
        dma(()),
        dma(()),
        dma((4 * planes,)),
        dma((chips, tp_n)),
        dma((3 * planes,)),
        dma((3, planes)),
        dma((planes,)),
        dma((planes,)),
    ]
    return pl.pallas_call(
        functools.partial(fused_kernel, (ep_n, tp_n, seq, quarter, colw, width)),
        out_shape=jax.ShapeDtypeStruct((seq, quarter), bf16),
        in_specs=specs,
        out_specs=pl.BlockSpec(memory_space=pltpu.VMEM),
        scratch_shapes=scratch,
        compiler_params=pltpu.CompilerParams(
            collective_id=0, has_side_effects=True, vmem_limit_bytes=60 * 1024 * 1024
        ),
        name="layer_step",
    )(*args)


def layer(*args):
    ep_n, tp_n = lax.axis_size("ep"), lax.axis_size("tp")
    if fits_fused(ep_n, tp_n, args[3].shape[1], args[1].shape[1], args[0].shape[1]):
        return fused_body(*args)
    return body(*args)


def solution(mesh):
    placed = (
        P("ep", "tp"),
        P("ep", "tp", None),
        P("tp"),
        P("tp", "ep"),
        P("tp", "ep"),
        P("tp", "ep"),
        P("tp", "ep"),
        P("tp", "ep"),
        P("tp"),
        P("tp"),
        P("tp"),
        P("tp", "ep"),
        P(),
        P("ep", None),
        P("ep", None),
        P("ep", None, "tp"),
        P("ep", None, "tp"),
        P("ep", "tp", None),
        P(None, "tp"),
        P(None, "tp"),
        P("tp", None),
    )
    return jax.shard_map(layer, mesh=mesh, in_specs=placed, out_specs=P("ep", "tp"), check_vma=False)
```
